32 devices in a mesh: ep: 16 (over z, y, core), tp: 2 (over x).
Axes of the slice: x: 2, y: 2, z: 4, core: 2. Of those that a mesh axis runs over, the one named last changes fastest.
Arguments:
- tokens: bfloat16 [128, 1024], P(('ep', 'tp')), may hold values from -6 to 6
- lengths: int32 [128], P('ep'), may hold values from 256 to 1024
- key_cache: bfloat16 [128, 1024, 128], P(('ep', 'tp')), may hold values from -1500 to 1500
- value_cache: bfloat16 [128, 1024, 128], P(('ep', 'tp')), may hold values from -6 to 6
- query_weight: bfloat16 [1024, 512], P(None, 'tp'), may hold values from -0.1875 to 0.1875
- key_weight: bfloat16 [1024, 128], replicated, may hold values from -0.1875 to 0.1875
- value_weight: bfloat16 [1024, 128], replicated, may hold values from -0.1875 to 0.1875
- lambdas: float32 [4], replicated, may hold values from 0.3 to 0.8
- head_gain: float32 [128], replicated, may hold values from 0.1 to 1.9
- output_weight: bfloat16 [512, 1024], P(None, 'tp'), may hold values from -0.25 to 0.25
- norm1_gain: float32 [1024], replicated, may hold values from 0.1 to 1.9
- routes: int32 [128, 6], P('ep'), may hold values from 0 to 15, all different within a row; in each aligned block of 8 rows (0 to 7, 8 to 15, ...) at most 6 rows name the same one
- route_logits: float32 [128, 6], P('ep'), may hold values from -9 to 410
- gate_weight: bfloat16 [16, 1024, 1024], P('ep', None, 'tp'), may hold values from -0.5 to 0.5
- up_weight: bfloat16 [16, 1024, 1024], P('ep', None, 'tp'), may hold values from -0.5 to 0.5
- down_weight: bfloat16 [16, 1024, 1024], P('ep', 'tp'), may hold values from -0.09375 to 0.09375
- norm2_gain: float32 [1024], replicated, may hold values from 0.1 to 1.9
Outputs:
- mixed: bfloat16 [128, 1024], P('ep', 'tp')
The draws below stay inside these ranges and needn't reach their ends.
Inputs may be any that keep to these rules, and one draw needn't show every extreme that they name: `routes`: in the 8 rows of each aligned block (the rows held by one index of ep) no expert is named by more than 6 rows, a bound that some block reaches; the experts of a row differ.
All inputs are finite; a program needn't handle non-finite values.
Results may differ from the reference program's by a relative error of at most 0.014.
Values may be sent and summed in bfloat16 or wider, within the bound.
No kernel may reach another device: no remote copies, remote signals or barrier semaphores. Data moves between devices by JAX's collectives and lax.ppermute only.
A program may use at most 64 MiB of HBM per device.

```python
import math
import jax
import jax.numpy as jnp
import numpy as np
from jax import lax

D = 1024
HEADS = 4
DH = 64
VH = 128
FF = 1024
TOPK = 6
CACHE = 1024
TOK_GRP = 8
BATCH = 128
EXPERTS = 16
CAP = 6
N_EP = 16
N_TP = 2


def draw_key_cache(key, part):
    base = jnp.clip(jax.random.normal(key, (BATCH, CACHE, 2 * DH), jnp.float32) * 1.75, -9.0, 9.0)
    return base.astype(jnp.bfloat16)


def draw_route_logits(key, part):
    base = jnp.clip(jax.random.normal(key, (BATCH, TOPK), jnp.float32) * 1.5, -9.0, 9.0)
    return base


def touch_ends(values, key, smallest, top_value):
    index_at = [jax.random.randint(jax.random.fold_in(key, axis), (), 0, length) for axis, length in enumerate(values.shape)]
    longest = values.shape.index(max(values.shape))
    neighbour = index_at[:longest] + [(index_at[longest] + 1) % values.shape[longest]] + index_at[longest + 1:]
    return values.at[tuple(index_at)].set(smallest).at[tuple(neighbour)].set(top_value)


def block_levels(key, extent, cuts, least, largest):
    level = 1.0
    for axis_at, parts in cuts:
        heights = jax.random.uniform(jax.random.fold_in(jax.random.fold_in(key, 6), axis_at), (parts,), jnp.float32, least / len(cuts), largest / len(cuts))
        level = level * jnp.repeat(jnp.exp(heights), extent[axis_at] // parts).reshape((-1,) + (1,) * (len(extent) - 1 - axis_at))
    return level


def deal_out(own_key, own, number, rows, amount, top, bound, lean):
    sequence = jax.random.permutation(own_key, amount)
    heavy_load, ordinary = load_shares(amount, rows * top, bound, lean, True), load_shares(amount, rows * top, bound, lean, False)
    places = jnp.arange(amount)

    def named(sizes, rotation):
        used = int((sizes > 0).sum())
        fixed = max(1, used // 4)
        moved = fixed + (places - fixed + rotation * (used - fixed)) % max(1, amount - fixed)
        return jnp.zeros((amount,), jnp.int32).at[sequence[jnp.where(places < fixed, places, moved)]].set(jnp.asarray(sizes, jnp.int32))

    sizes = jnp.where(number % 4 == 0, named(heavy_load, number // 4), named(ordinary, number - number // 4 - 1))
    mixed = jax.random.permutation(jax.random.fold_in(own, 3), amount)
    source_of, receiver = mixed[0:amount // 2 * 2:2], mixed[1:amount // 2 * 2:2]
    room = jnp.minimum(sizes[source_of] - 1, bound - sizes[receiver]) // 2
    room = jnp.where((source_of == sequence[0]) | (receiver == sequence[0]) | (sizes[receiver] == 0), 0, jnp.maximum(room, 0))
    moved = jax.random.randint(jax.random.fold_in(own, 4), (amount // 2,), 0, 1 << 20) % (room + 1)
    sizes = sizes.at[source_of].add(-moved).at[receiver].add(moved)
    members = jnp.searchsorted(jnp.cumsum(sizes), jnp.arange(rows * top), side="right").astype(jnp.int32)
    grid = members.reshape(top, rows).T
    grid = grid[jax.random.permutation(jax.random.fold_in(own, 1), rows)]
    rotation = jax.random.randint(jax.random.fold_in(own, 2), (rows, 1), 0, top)
    return jnp.take_along_axis(grid, (jnp.arange(top)[None, :] + rotation) % top, axis=1)


def load_shares(number_of, total, reach, skew, full):
    weights = [(1 << 20) // math.isqrt(grade ** skew) + 1 for grade in range(1, number_of + 1)]
    largest = reach if full else min(reach, max(-(-total // number_of), total * weights[0] // sum(weights)))
    least = 1 if total - largest >= number_of - 1 else 0
    given, rest = [largest] + [least] * (number_of - 1), total - largest - least * (number_of - 1)
    while rest > 0:
        candidates = [i for i in range(1, number_of) if given[i] < largest] or [i for i in range(1, number_of) if given[i] < reach]
        whole, budget = sum([weights[i] for i in candidates]), rest
        for i in candidates:
            more = min(reach - given[i], max(1, budget * weights[i] // whole), rest)
            given[i] = given[i] + more
            rest = rest - more
    return np.array(given)


def gaussian(key, shape, scale, most, cuts=(), kind=jnp.bfloat16):
    entries = jax.random.normal(key, shape, jnp.float32) * scale
    if len(cuts) > 0:
        entries = block_levels(key, shape, cuts, -0.22, 0.18) * entries
    return jnp.clip(entries, min=-most, max=most).astype(kind)


def setup_inputs(seed: int = 0) -> dict:
    key_list = jax.random.split(jax.random.key(seed), 18)
    tokens = gaussian(key_list[0], (BATCH, D), 1.0, 6.0, ((0, 32),))
    lengths = touch_ends(jax.random.randint(key_list[1], (BATCH,), CACHE // 4, CACHE + 1), jax.random.fold_in(key_list[1], 1), CACHE // 4, CACHE).astype(jnp.int32)
    key_cache = draw_key_cache(jax.random.fold_in(key_list[17], 71), 0)
    value_cache = gaussian(key_list[3], (BATCH, CACHE, VH), 1.0, 6.0, ((0, 32),))
    query_weight = gaussian(key_list[4], (D, 2 * DH * HEADS), D ** -0.5, 0.1875, ((1, 2),))
    key_weight = gaussian(key_list[5], (D, 2 * DH), D ** -0.5, 0.1875)
    value_weight = gaussian(key_list[6], (D, VH), D ** -0.5, 0.1875)
    lambdas = jnp.clip(jax.random.uniform(key_list[7], (HEADS,), jnp.float32, 0.3, 0.8), 0.3, 0.8)
    head_gain = jnp.clip(1.0 + 0.18 * jax.random.normal(key_list[8], (VH,), jnp.float32), 0.1, 1.9)
    output_weight = gaussian(key_list[9], (HEADS * VH, D), (HEADS * VH) ** -0.5, 0.25, ((1, 2),))
    norm1_gain = jnp.clip(1.0 + 0.18 * jax.random.normal(key_list[10], (D,), jnp.float32), 0.1, 1.9)
    routes_keys = jax.random.split(jax.random.fold_in(key_list[11], 1), BATCH // TOK_GRP)
    routes_turns = jax.random.permutation(jax.random.fold_in(key_list[11], 3), BATCH // TOK_GRP)
    routes = jax.vmap(lambda own, number: deal_out(jax.random.fold_in(key_list[11], 2), own, number, TOK_GRP, EXPERTS, TOPK, CAP, 2))(routes_keys, routes_turns).reshape((BATCH, TOPK))
    route_logits = draw_route_logits(jax.random.fold_in(key_list[17], 71), 0)
    gate_weight = gaussian(key_list[13], (EXPERTS, D, FF), (D // 9) ** -0.5, 0.5, ((0, 16), (2, 2)))
    up_weight = gaussian(key_list[14], (EXPERTS, D, FF), (D // 9) ** -0.5, 0.5, ((0, 16), (2, 2)))
    down_weight = gaussian(key_list[15], (EXPERTS, FF, D), (4 * FF) ** -0.5, 0.09375, ((0, 16), (1, 2)))
    norm2_gain = jnp.clip(1.0 + 0.18 * jax.random.normal(key_list[16], (D,), jnp.float32), 0.1, 1.9)
    return {"tokens": tokens, "lengths": lengths, "key_cache": key_cache, "value_cache": value_cache, "query_weight": query_weight, "key_weight": key_weight, "value_weight": value_weight, "lambdas": lambdas, "head_gain": head_gain, "output_weight": output_weight, "norm1_gain": norm1_gain, "routes": routes, "route_logits": route_logits, "gate_weight": gate_weight, "up_weight": up_weight, "down_weight": down_weight, "norm2_gain": norm2_gain}


ALPHA = 1.4142135623730951
EPS = 1e-05
THETA = 500000.0
LIMIT = 7.0
SLOPE = 1.702

def rotate(values, positions):
    half = values.shape[-1] // 2
    freqs = THETA ** (-jnp.arange(half, dtype=jnp.float32) / half)
    angles = positions.astype(jnp.float32)[:, None] * freqs[None, :]
    shape = (angles.shape[0],) + (1,) * (values.ndim - 2) + (half,)
    cosine = jnp.cos(angles).reshape(shape)
    sine = jnp.sin(angles).reshape(shape)
    first = values[..., :half]
    second = values[..., half:]
    return jnp.concatenate([first * cosine - second * sine, second * cosine + first * sine], axis=-1)

def norm_rows(summed, gain):
    mean = lax.optimization_barrier(jnp.mean(summed, axis=-1, keepdims=True))
    center = summed - mean
    spread = lax.optimization_barrier(jnp.mean(center * center, axis=-1, keepdims=True))
    return center * lax.rsqrt(spread + EPS) * gain

def choose_slots(routes_block, experts, capacity):
    flat = routes_block.reshape(-1).astype(jnp.int32)
    onehot = (flat[:, None] == jnp.arange(experts, dtype=jnp.int32)[None, :]).astype(jnp.int32)
    before = jnp.cumsum(onehot, axis=0) - onehot
    slot = lax.optimization_barrier(jnp.sum(before * onehot, axis=1))
    target = flat * capacity + slot
    return target[:, None] == jnp.arange(experts * capacity, dtype=jnp.int32)[None, :]

def attend_block(query, new_key, new_value, keys, values, lengths, lambdas, head_gain):
    f32 = jnp.float32
    count, length = (keys.shape[0], keys.shape[1])
    keys = keys.reshape(count, length, 2, -1)
    scale = keys.shape[-1] ** (-0.5)
    past = jnp.einsum('bhmd,bjmd->bhmj', query.astype(f32), keys.astype(f32)) * scale
    live = jnp.arange(length, dtype=jnp.int32)[None, :] < lengths[:, None]
    past = jnp.where(live[:, None, None, :], past, -jnp.inf)
    selfs = jnp.einsum('bhmd,bmd->bhm', query.astype(f32), new_key.astype(f32)) * scale
    top = jnp.maximum(lax.optimization_barrier(jnp.max(past, axis=-1)), selfs)
    past_exp = jnp.exp(past - top[..., None])
    self_exp = jnp.exp(selfs - top)
    total = lax.optimization_barrier(jnp.sum(past_exp, axis=-1)) + self_exp
    past_prob = past_exp / total[..., None]
    self_prob = self_exp / total
    mixing = lambdas[None, :]
    past_weight = (past_prob[:, :, 0] - mixing[..., None] * past_prob[:, :, 1]).astype(jnp.bfloat16)
    self_weight = (self_prob[:, :, 0] - mixing * self_prob[:, :, 1]).astype(jnp.bfloat16)
    head_out = jnp.einsum('bhj,bje->bhe', past_weight.astype(f32), values.astype(f32))
    head_out = head_out + self_weight.astype(f32)[..., None] * new_value.astype(f32)[:, None, :]
    normed = head_out * lax.rsqrt(lax.optimization_barrier(jnp.mean(head_out * head_out, axis=-1, keepdims=True)) + EPS) * head_gain
    return normed.astype(jnp.bfloat16).reshape(count, -1)

def reference(tokens, lengths, key_cache, value_cache, query_weight, key_weight, value_weight, lambdas, head_gain, output_weight, norm1_gain, routes, route_logits, gate_weight, up_weight, down_weight, norm2_gain):
    f32 = jnp.float32
    bf16 = jnp.bfloat16
    rows = tokens.shape[0]
    query = jnp.dot(tokens, query_weight, preferred_element_type=f32).reshape(rows, HEADS, 2, DH)
    query = rotate(query, lengths).astype(bf16)
    new_key = jnp.dot(tokens, key_weight, preferred_element_type=f32).reshape(rows, 2, DH)
    new_key = rotate(new_key, lengths).astype(bf16)
    new_value = jnp.dot(tokens, value_weight, preferred_element_type=f32).astype(bf16)

    def one_group(pieces):
        return attend_block(*pieces, lambdas, head_gain)
    grouped = tuple((a.reshape((N_EP, TOK_GRP) + a.shape[1:]) for a in (query, new_key, new_value, key_cache, value_cache, lengths)))
    attended = lax.map(one_group, grouped).reshape(rows, HEADS * VH)
    summed = ALPHA * tokens.astype(f32) + jnp.dot(attended, output_weight, preferred_element_type=f32)
    settled = norm_rows(summed, norm1_gain).astype(bf16)
    route_weight = jax.nn.softmax(route_logits, axis=-1)
    routes_grouped = routes.reshape(N_EP, TOK_GRP, TOPK)

    def dispatch(pieces):
        rows_block, routes_block = pieces
        chosen = choose_slots(routes_block, EXPERTS, CAP)
        placing = lax.optimization_barrier(jnp.sum(chosen.reshape(TOK_GRP, TOPK, -1).astype(f32), axis=1)).astype(bf16)
        sent = jnp.dot(placing.T, rows_block, preferred_element_type=f32)
        return sent.astype(bf16)
    sends = lax.map(dispatch, (settled.reshape(N_EP, TOK_GRP, D), routes_grouped))
    sends = jnp.moveaxis(sends.reshape(N_EP, EXPERTS, CAP, D), 1, 0)
    block = FF // N_TP

    def run_expert(pieces):
        rows_e, gate_e, up_e, down_e = pieces
        gate_h = jnp.einsum('scd,df->scf', rows_e.astype(f32), gate_e.astype(f32))
        up_h = jnp.einsum('scd,df->scf', rows_e.astype(f32), up_e.astype(f32))
        clipped = jnp.minimum(gate_h, LIMIT)
        linear = jnp.clip(up_h, -LIMIT, LIMIT)
        act = (clipped * jax.nn.sigmoid(SLOPE * clipped) * (linear + 1.0)).astype(bf16)
        total = jnp.zeros(rows_e.shape, f32)
        for index in range(N_TP):
            piece = jnp.einsum('scf,fd->scd', act[..., index * block:(index + 1) * block].astype(f32), down_e[index * block:(index + 1) * block].astype(f32))
            rounded = lax.optimization_barrier(piece.astype(bf16))
            total = total + rounded.astype(f32)
        return total.astype(bf16)
    answers = lax.map(run_expert, (sends, gate_weight, up_weight, down_weight))
    answers = jnp.moveaxis(answers, 1, 0).reshape(N_EP, EXPERTS * CAP, D)

    def combine(pieces):
        answers_block, routes_block = pieces
        chosen = choose_slots(routes_block, EXPERTS, CAP)
        picked = jnp.dot(chosen.astype(bf16), answers_block, preferred_element_type=f32)
        return picked.reshape(TOK_GRP, TOPK, D)
    picked = lax.map(combine, (answers, routes_grouped)).reshape(rows, TOPK, D)
    routed = lax.optimization_barrier(jnp.sum(picked * route_weight[:, :, None], axis=1))
    return norm_rows(ALPHA * settled.astype(f32) + routed, norm2_gain).astype(bf16)
```

```python
import jax
import jax.numpy as jnp
from jax import lax
from jax.sharding import PartitionSpec as P

ALPHA = 1.4142135623730951
EPS = 1e-05
THETA = 500000.0
LIMIT = 7.0
SLOPE = 1.702
LANES = 128


def rotate(values, positions):
    half = values.shape[-1] // 2
    freqs = THETA ** (-jnp.arange(half, dtype=jnp.float32) / half)
    angles = positions.astype(jnp.float32)[:, None] * freqs[None, :]
    shape = (angles.shape[0],) + (1,) * (values.ndim - 2) + (half,)
    cosine = jnp.cos(angles).reshape(shape)
    sine = jnp.sin(angles).reshape(shape)
    first = values[..., :half]
    second = values[..., half:]
    return jnp.concatenate(
        [first * cosine - second * sine, second * cosine + first * sine], axis=-1
    )


def norm_rows(summed, gain):
    mean = jnp.mean(summed, axis=-1, keepdims=True)
    center = summed - mean
    spread = jnp.mean(center * center, axis=-1, keepdims=True)
    return center * lax.rsqrt(spread + EPS) * gain


def swap(values):
    return lax.ppermute(values, "tp", [(0, 1), (1, 0)])


def joined(mine, other, rank, axis):
    first = rank == 0
    return jnp.concatenate(
        [jnp.where(first, mine, other), jnp.where(first, other, mine)], axis=axis
    )


def gather_tp(values):
    if lax.axis_size("tp") == 2:
        return joined(values, swap(values), lax.axis_index("tp"), 0)
    return lax.all_gather(values, "tp", axis=0, tiled=True)


def regroup_tp(values, own):
    if lax.axis_size("tp") == 2:
        rank = lax.axis_index("tp")
        other = swap(lax.dynamic_slice_in_dim(values, (1 - rank) * own, own))
        return joined(lax.dynamic_slice_in_dim(values, rank * own, own), other, rank, 1)
    return lax.all_to_all(values, "tp", split_axis=0, concat_axis=1, tiled=True)


def sum_tp(values):
    if lax.axis_size("tp") == 2:
        return values + swap(values.astype(jnp.bfloat16)).astype(jnp.float32)
    return lax.psum(values, "tp")


def body(
    tokens,
    lengths,
    key_cache,
    value_cache,
    query_weight,
    key_weight,
    value_weight,
    lambdas,
    head_gain,
    output_weight,
    norm1_gain,
    routes,
    route_logits,
    gate_weight,
    up_weight,
    down_weight,
    norm2_gain,
):
    bf16 = jnp.bfloat16
    f32 = jnp.float32
    tp_count = lax.axis_size("tp")
    tp_rank = lax.axis_index("tp")
    experts = lax.axis_size("ep")
    ep_rank = lax.axis_index("ep")
    own, width = tokens.shape
    group = own * tp_count
    part = width // tp_count
    heads = lambdas.shape[0]
    head_dim = key_weight.shape[1] // 2
    length = key_cache.shape[1]
    group_rows = gather_tp(tokens)
    query = jnp.dot(group_rows, query_weight, preferred_element_type=f32).reshape(
        group, -1, 2, head_dim
    )
    query = rotate(query, lengths).astype(bf16).reshape(group, -1)
    query = regroup_tp(query, own).reshape(own, heads, 2, head_dim)
    own_lengths = lax.dynamic_slice_in_dim(lengths, tp_rank * own, own)
    new_key = jnp.dot(tokens, key_weight, preferred_element_type=f32).reshape(own, 2, head_dim)
    new_key = rotate(new_key, own_lengths).astype(bf16).reshape(own, 2 * head_dim)
    new_value = jnp.dot(tokens, value_weight, preferred_element_type=f32).astype(bf16)
    scale = head_dim ** (-0.5)
    blank = jnp.zeros((own, heads, head_dim), bf16)
    wide = jnp.concatenate(
        [
            jnp.concatenate([query[:, :, 0], blank], axis=-1),
            jnp.concatenate([blank, query[:, :, 1]], axis=-1),
        ],
        axis=1,
    )
    past = jnp.einsum("bqd,bjd->bqj", wide, key_cache, preferred_element_type=f32) * scale
    live = jnp.arange(length, dtype=jnp.int32)[None, :] < own_lengths[:, None]
    past = jnp.where(live[:, None, :], past, -jnp.inf)
    selfs = jnp.sum(wide.astype(f32) * new_key.astype(f32)[:, None, :], axis=-1) * scale
    top = jnp.maximum(jnp.max(past, axis=-1), selfs)
    past_exp = jnp.exp(past - top[..., None])
    self_exp = jnp.exp(selfs - top)
    total = jnp.sum(past_exp, axis=-1) + self_exp
    past_prob = past_exp / total[..., None]
    self_prob = self_exp / total
    mixing = lambdas[None, :]
    past_weight = (past_prob[:, :heads] - mixing[..., None] * past_prob[:, heads:]).astype(bf16)
    self_weight = (self_prob[:, :heads] - mixing * self_prob[:, heads:]).astype(bf16)
    head_out = jnp.einsum("bhj,bje->bhe", past_weight, value_cache, preferred_element_type=f32)
    head_out = head_out + self_weight.astype(f32)[..., None] * new_value.astype(f32)[:, None, :]
    normed = (
        head_out
        * lax.rsqrt(jnp.mean(head_out * head_out, axis=-1, keepdims=True) + EPS)
        * head_gain
    )
    attended = normed.astype(bf16).reshape(own, -1)
    mix = jnp.dot(gather_tp(attended), output_weight, preferred_element_type=f32)
    column_start = tp_rank * part
    own_columns = lax.dynamic_slice_in_dim(group_rows, column_start, part, 1).astype(f32)
    summed = ALPHA * own_columns + mix
    part_mean = jnp.mean(summed, axis=1, keepdims=True)
    mean_high = part_mean.astype(bf16)
    mean_low = (part_mean - mean_high.astype(f32)).astype(bf16)
    lane = jnp.arange(LANES, dtype=jnp.int32)[None, :]
    extra = jnp.where(lane == 0, mean_high, jnp.where(lane == 1, mean_low, jnp.zeros((), bf16)))
    packed = jnp.concatenate([(summed - part_mean).astype(bf16), extra], axis=1)
    packed = jnp.broadcast_to(packed[None], (experts * tp_count,) + packed.shape)
    packed = lax.all_to_all(packed, ("ep", "tp"), split_axis=0, concat_axis=0, tiled=True)
    packed = packed.reshape(experts, tp_count, group, part + LANES).astype(f32)
    pieces = packed[..., :part] + (packed[..., part] + packed[..., part + 1])[..., None]
    everyone = jnp.concatenate([pieces[:, index] for index in range(tp_count)], axis=-1)
    settled = norm_rows(everyone, norm1_gain).astype(bf16)
    rows = settled.reshape(experts * group, width)
    gate_h = jnp.dot(rows, gate_weight[0], preferred_element_type=f32)
    up_h = jnp.dot(rows, up_weight[0], preferred_element_type=f32)
    clipped = jnp.minimum(gate_h, LIMIT)
    linear = jnp.clip(up_h, -LIMIT, LIMIT)
    act = (clipped * jax.nn.sigmoid(SLOPE * clipped) * (linear + 1.0)).astype(bf16)
    terms = jnp.dot(act, down_weight[0], preferred_element_type=f32).astype(bf16)
    terms = terms.reshape(experts, group, width)
    back = lax.all_to_all(terms, "ep", split_axis=0, concat_axis=0, tiled=True)
    route_weight = jax.nn.softmax(route_logits, axis=-1)
    names = jnp.arange(experts, dtype=jnp.int32)[:, None, None]
    dense = jnp.sum(jnp.where(routes[None] == names, route_weight[None], 0.0), axis=-1)
    routed = sum_tp(jnp.sum(back.astype(f32) * dense[:, :, None], axis=0))
    own_settled = lax.dynamic_index_in_dim(settled, ep_rank, 0, keepdims=False)
    final = ALPHA * own_settled.astype(f32) + routed
    mean = jnp.mean(final, axis=-1, keepdims=True)
    spread = jnp.mean((final - mean) * (final - mean), axis=-1, keepdims=True)
    own_final = lax.dynamic_slice_in_dim(final, column_start, part, 1)
    gain = lax.dynamic_slice_in_dim(norm2_gain, column_start, part)
    return ((own_final - mean) * lax.rsqrt(spread + EPS) * gain).astype(bf16)


def solution(mesh):
    in_specs = (
        P(("ep", "tp"), None),
        P("ep"),
        P(("ep", "tp"), None, None),
        P(("ep", "tp"), None, None),
        P(None, "tp"),
        P(),
        P(),
        P(),
        P(),
        P(None, "tp"),
        P(),
        P("ep", None),
        P("ep", None),
        P("ep", None, "tp"),
        P("ep", None, "tp"),
        P("ep", "tp", None),
        P(),
    )
    out_specs = P("ep", "tp")
    return jax.shard_map(body, mesh=mesh, in_specs=in_specs, out_specs=out_specs, check_vma=False)
```

```python
import jax
import jax.numpy as jnp
from jax import lax
from jax.experimental import pallas as pl
from jax.experimental.pallas import tpu as pltpu
from jax.sharding import PartitionSpec as P

ALPHA = 1.4142135623730951
EPS = 1e-05
THETA = 500000.0
LIMIT = 7.0
SLOPE = 1.702
LANES = 128


def turns(positions, half):
    freqs = THETA ** (-jnp.arange(half, dtype=jnp.float32) / half)
    angles = positions.astype(jnp.float32)[:, None] * freqs[None, :]
    return jnp.cos(angles), jnp.sin(angles)


def rotate(values, cosine, sine):
    half = cosine.shape[-1]
    shape = (cosine.shape[0],) + (1,) * (values.ndim - 2) + (half,)
    cosine = cosine.reshape(shape)
    sine = sine.reshape(shape)
    first = values[..., :half]
    second = values[..., half:]
    return jnp.concatenate(
        [first * cosine - second * sine, second * cosine + first * sine], axis=-1
    )


def norm_rows(summed, gain):
    mean = jnp.mean(summed, axis=-1, keepdims=True)
    center = summed - mean
    spread = jnp.mean(center * center, axis=-1, keepdims=True)
    return center * lax.rsqrt(spread + EPS) * gain


def swap(values):
    return lax.ppermute(values, "tp", [(0, 1), (1, 0)])


def joined(mine, other, rank, axis):
    first = rank == 0
    return jnp.concatenate(
        [jnp.where(first, mine, other), jnp.where(first, other, mine)], axis=axis
    )


def gather_tp(values):
    if lax.axis_size("tp") == 2:
        return joined(values, swap(values), lax.axis_index("tp"), 0)
    return lax.all_gather(values, "tp", axis=0, tiled=True)


def vmem():
    return pl.BlockSpec(memory_space=pltpu.VMEM)


def smem():
    return pl.BlockSpec(memory_space=pltpu.SMEM)


def room(*arrays, extra):
    need = 2 * sum(a.size * a.dtype.itemsize for a in arrays) + extra
    return pltpu.CompilerParams(vmem_limit_bytes=min(need, 60 << 20))


def attend_kernel(
    lengths, query, new_key, new_value, key_cache, value_cache, lambdas, head_gain, attended
):
    f32 = jnp.float32
    bf16 = jnp.bfloat16
    own, length, both = key_cache.shape
    heads = lambdas.shape[0]
    scale = (both // 2) ** (-0.5)
    queries = query[...].astype(f32)
    keys = new_key[...].astype(f32)
    values = new_value[...].astype(f32)
    mixing = lambdas[...]
    low = lax.broadcasted_iota(jnp.int32, (heads, both), 1) < both // 2
    place = lax.broadcasted_iota(jnp.int32, (2 * heads, length), 1)
    past = []
    selfs = []
    for b in range(own):
        maps = jnp.concatenate(
            [queries[b : b + 1, h * both : (h + 1) * both] for h in range(heads)], axis=0
        )
        wide = jnp.concatenate([jnp.where(low, maps, 0.0), jnp.where(low, 0.0, maps)], axis=0)
        scores = lax.dot_general(
            wide.astype(bf16),
            key_cache[b],
            (((1,), (1,)), ((), ())),
            preferred_element_type=f32,
        )
        past.append(jnp.where(place < lengths[b], scores * scale, -jnp.inf))
        selfs.append(jnp.sum(wide * keys[b : b + 1], axis=-1, keepdims=True) * scale)
    past = jnp.concatenate(past, axis=0)
    selfs = jnp.concatenate(selfs, axis=0)
    top = jnp.maximum(jnp.max(past, axis=-1, keepdims=True), selfs)
    past_exp = jnp.exp(past - top)
    self_exp = jnp.exp(selfs - top)
    share = 1.0 / (jnp.sum(past_exp, axis=-1, keepdims=True) + self_exp)
    past_prob = past_exp * share
    self_prob = self_exp * share
    outs = []
    for b in range(own):
        first, second, last = 2 * heads * b, 2 * heads * b + heads, 2 * heads * (b + 1)
        past_weight = (past_prob[first:second] - mixing * past_prob[second:last]).astype(bf16)
        self_weight = (self_prob[first:second] - mixing * self_prob[second:last]).astype(bf16)
        head_out = jnp.dot(past_weight, value_cache[b], preferred_element_type=f32)
        outs.append(head_out + self_weight.astype(f32) * values[b : b + 1])
    head_out = jnp.concatenate(outs, axis=0)
    spread = jnp.mean(head_out * head_out, axis=-1, keepdims=True)
    normed = head_out * lax.rsqrt(spread + EPS) * head_gain[...]
    rows = [
        jnp.concatenate([normed[b * heads + h : b * heads + h + 1] for h in range(heads)], axis=1)
        for b in range(own)
    ]
    attended[...] = jnp.concatenate(rows, axis=0).astype(bf16)


def expert_kernel(packed, gain, gate_weight, up_weight, down_weight, settled, terms):
    f32 = jnp.float32
    bf16 = jnp.bfloat16
    experts, tp_count, group, lanes = packed.shape
    part = lanes - LANES
    pieces = []
    for index in range(tp_count):
        piece = packed[:, index].astype(f32).reshape(experts * group, lanes)
        pieces.append(piece[:, :part] + (piece[:, part : part + 1] + piece[:, part + 1 : part + 2]))
    rows = norm_rows(jnp.concatenate(pieces, axis=1), gain[...]).astype(bf16)
    settled[...] = rows
    gate_h = jnp.dot(rows, gate_weight[...], preferred_element_type=f32)
    up_h = jnp.dot(rows, up_weight[...], preferred_element_type=f32)
    clipped = jnp.minimum(gate_h, LIMIT)
    linear = jnp.clip(up_h, -LIMIT, LIMIT)
    act = (clipped * jax.nn.sigmoid(SLOPE * clipped) * (linear + 1.0)).astype(bf16)
    terms[...] = jnp.dot(act, down_weight[...], preferred_element_type=f32).astype(bf16)


def final_kernel(rank, settled, mine, other, gain, result, whole):
    f32 = jnp.float32
    part = result.shape[1]
    final = ALPHA * settled[...].astype(f32) + (mine[...] + other[...].astype(f32))
    mean = jnp.mean(final, axis=-1, keepdims=True)
    spread = jnp.mean((final - mean) * (final - mean), axis=-1, keepdims=True)
    whole[...] = (final - mean) * lax.rsqrt(spread + EPS) * gain[...]
    start = pl.multiple_of(rank[0] * part, LANES)
    result[...] = whole[:, pl.ds(start, part)].astype(jnp.bfloat16)


def body(
    tokens,
    lengths,
    key_cache,
    value_cache,
    query_weight,
    key_weight,
    value_weight,
    lambdas,
    head_gain,
    output_weight,
    norm1_gain,
    routes,
    route_logits,
    gate_weight,
    up_weight,
    down_weight,
    norm2_gain,
):
    bf16 = jnp.bfloat16
    f32 = jnp.float32
    tp_count = lax.axis_size("tp")
    tp_rank = lax.axis_index("tp")
    experts = lax.axis_size("ep")
    ep_rank = lax.axis_index("ep")
    own, width = tokens.shape
    group = own * tp_count
    part = width // tp_count
    heads = lambdas.shape[0]
    head_dim = key_weight.shape[1] // 2
    columns = query_weight.shape[1]
    cosine, sine = turns(lengths, head_dim // 2)
    own_turn = [lax.dynamic_slice_in_dim(t, tp_rank * own, own) for t in (cosine, sine)]
    if tp_count == 2:
        others = swap(tokens)
        peer_turn = [lax.dynamic_slice_in_dim(t, (1 - tp_rank) * own, own) for t in (cosine, sine)]
        sent = jnp.dot(others, query_weight, preferred_element_type=f32)
        sent = rotate(sent.reshape(own, -1, 2, head_dim), *peer_turn).astype(bf16)
        sent = sent.reshape(own, columns)
        late, sent = lax.optimization_barrier((tokens, sent))
        came = swap(sent)
        kept = jnp.dot(late, query_weight, preferred_element_type=f32)
        kept = rotate(kept.reshape(own, -1, 2, head_dim), *own_turn).astype(bf16)
        query = joined(kept.reshape(own, columns), came, tp_rank, 1)
        group_rows = joined(late, others, tp_rank, 0)
    else:
        late = tokens
        group_rows = lax.all_gather(tokens, "tp", axis=0, tiled=True)
        query = jnp.dot(group_rows, query_weight, preferred_element_type=f32)
        query = rotate(query.reshape(group, -1, 2, head_dim), cosine, sine).astype(bf16)
        query = lax.all_to_all(
            query.reshape(group, columns), "tp", split_axis=0, concat_axis=1, tiled=True
        )
    own_lengths = lax.dynamic_slice_in_dim(lengths, tp_rank * own, own)
    new_key = jnp.dot(late, key_weight, preferred_element_type=f32)
    new_key = new_key.reshape(own, 2, head_dim)
    new_key = rotate(new_key, *own_turn).astype(bf16).reshape(own, 2 * head_dim)
    new_value = jnp.dot(late, value_weight, preferred_element_type=f32).astype(bf16)
    attended = pl.pallas_call(
        attend_kernel,
        out_shape=jax.ShapeDtypeStruct((own, heads * value_cache.shape[2]), bf16),
        in_specs=[smem()] + [vmem()] * 7,
        out_specs=vmem(),
        compiler_params=room(key_cache, value_cache, extra=2 << 20),
        name="attend",
    )(
        own_lengths,
        query,
        new_key,
        new_value,
        key_cache,
        value_cache,
        lambdas.reshape(heads, 1),
        head_gain.reshape(1, -1),
    )
    zero = attended[0, 0].astype(f32) * 0.0
    gains = jnp.stack([norm1_gain, norm2_gain]) + zero
    gains = lax.optimization_barrier(gains)
    gathered = gather_tp(attended)
    mix = jnp.dot(gathered, output_weight, preferred_element_type=f32)
    column_start = tp_rank * part
    own_columns = lax.dynamic_slice_in_dim(group_rows, column_start, part, 1).astype(f32)
    summed = ALPHA * own_columns + mix
    part_mean = jnp.mean(summed, axis=1, keepdims=True)
    mean_high = part_mean.astype(bf16)
    mean_low = (part_mean - mean_high.astype(f32)).astype(bf16)
    lane = jnp.arange(LANES, dtype=jnp.int32)[None, :]
    extra = jnp.where(lane == 0, mean_high, jnp.where(lane == 1, mean_low, jnp.zeros((), bf16)))
    packed = jnp.concatenate([(summed - part_mean).astype(bf16), extra], axis=1)
    packed = jnp.broadcast_to(packed[None], (experts * tp_count,) + packed.shape)
    packed = lax.all_to_all(packed, ("ep", "tp"), split_axis=0, concat_axis=0, tiled=True)
    settled, terms = pl.pallas_call(
        expert_kernel,
        out_shape=(jax.ShapeDtypeStruct((experts * group, width), bf16),) * 2,
        in_specs=[vmem()] * 5,
        out_specs=(vmem(), vmem()),
        compiler_params=room(
            packed, gate_weight, up_weight, down_weight, extra=24 * experts * group * width
        ),
        name="expert",
    )(
        packed.reshape(experts, tp_count, group, part + LANES),
        gains[0:1],
        gate_weight[0],
        up_weight[0],
        down_weight[0],
    )
    terms = terms.reshape(experts, group, width)
    back = lax.all_to_all(terms, "ep", split_axis=0, concat_axis=0, tiled=True)
    route_weight = jax.nn.softmax(route_logits, axis=-1)
    names = jnp.arange(experts, dtype=jnp.int32)[:, None, None]
    dense = jnp.sum(jnp.where(routes[None] == names, route_weight[None], 0.0), axis=-1)
    mine = jnp.sum(back.astype(f32) * dense[:, :, None], axis=0)
    if tp_count == 2:
        other = swap(mine.astype(bf16))
    else:
        other = lax.psum(mine, "tp") - mine
    own_settled = lax.dynamic_slice_in_dim(settled, ep_rank * group, group)
    return pl.pallas_call(
        final_kernel,
        out_shape=jax.ShapeDtypeStruct((group, part), bf16),
        in_specs=[smem()] + [vmem()] * 4,
        out_specs=vmem(),
        scratch_shapes=[pltpu.VMEM((group, width), f32)],
        compiler_params=room(mine, mine, mine, extra=1 << 20),
        name="final",
    )(tp_rank.reshape(1), own_settled, mine, other, gains[1:2])


def solution(mesh):
    in_specs = (
        P(("ep", "tp"), None),
        P("ep"),
        P(("ep", "tp"), None, None),
        P(("ep", "tp"), None, None),
        P(None, "tp"),
        P(),
        P(),
        P(),
        P(),
        P(None, "tp"),
        P(),
        P("ep", None),
        P("ep", None),
        P("ep", None, "tp"),
        P("ep", None, "tp"),
        P("ep", "tp", None),
        P(),
    )
    out_specs = P("ep", "tp")

    return jax.shard_map(body, mesh=mesh, in_specs=in_specs, out_specs=out_specs, check_vma=False)
```

```python
import jax
import jax.numpy as jnp
from jax import lax
from jax.experimental import pallas as pl
from jax.experimental.pallas import tpu as pltpu
from jax.sharding import PartitionSpec as P

ALPHA = 1.4142135623730951
EPS = 1e-05
THETA = 500000.0
LIMIT = 7.0
SLOPE = 1.702
LANES = 128


def turns(positions, half):
    freqs = THETA ** (-jnp.arange(half, dtype=jnp.float32) / half)
    angles = positions.astype(jnp.float32)[:, None] * freqs[None, :]
    return jnp.cos(angles), jnp.sin(angles)


def rotate(values, cosine, sine):
    half = cosine.shape[-1]
    shape = (cosine.shape[0],) + (1,) * (values.ndim - 2) + (half,)
    cosine = cosine.reshape(shape)
    sine = sine.reshape(shape)
    first = values[..., :half]
    second = values[..., half:]
    return jnp.concatenate(
        [first * cosine - second * sine, second * cosine + first * sine], axis=-1
    )


def norm_rows(summed, gain):
    mean = jnp.mean(summed, axis=-1, keepdims=True)
    center = summed - mean
    spread = jnp.mean(center * center, axis=-1, keepdims=True)
    return center * lax.rsqrt(spread + EPS) * gain


def swap(values):
    return lax.ppermute(values, "tp", [(0, 1), (1, 0)])


def joined(mine, other, rank, axis):
    first = rank == 0
    return jnp.concatenate(
        [jnp.where(first, mine, other), jnp.where(first, other, mine)], axis=axis
    )


def gather_tp(values):
    if lax.axis_size("tp") == 2:
        return joined(values, swap(values), lax.axis_index("tp"), 0)
    return lax.all_gather(values, "tp", axis=0, tiled=True)


def vmem():
    return pl.BlockSpec(memory_space=pltpu.VMEM)


def smem():
    return pl.BlockSpec(memory_space=pltpu.SMEM)


def away():
    return pl.BlockSpec(memory_space=pltpu.HBM)


def room(*arrays, extra):
    need = 2 * sum(a.size * a.dtype.itemsize for a in arrays) + extra
    return pltpu.CompilerParams(vmem_limit_bytes=min(need, 60 << 20))


def attend_kernel(
    lengths,
    query,
    new_key,
    tokens,
    key_cache,
    lambdas,
    value_weight,
    value_cache,
    head_gain,
    attended,
    weight_here,
    cache_here,
    gain_here,
    arrived,
):
    f32 = jnp.float32
    bf16 = jnp.bfloat16
    own, length, both = key_cache.shape
    heads = lambdas.shape[0]
    copies = [
        pltpu.make_async_copy(value_weight, weight_here, arrived.at[0]),
        pltpu.make_async_copy(value_cache, cache_here, arrived.at[1]),
        pltpu.make_async_copy(head_gain, gain_here, arrived.at[2]),
    ]
    for copy in copies:
        copy.start()
    scale = (both // 2) ** (-0.5)
    queries = query[...].astype(f32)
    keys = new_key[...].astype(f32)
    mixing = lambdas[...]
    low = lax.broadcasted_iota(jnp.int32, (heads, both), 1) < both // 2
    place = lax.broadcasted_iota(jnp.int32, (2 * heads, length), 1)
    past = []
    selfs = []
    for b in range(own):
        maps = jnp.concatenate(
            [queries[b : b + 1, h * both : (h + 1) * both] for h in range(heads)], axis=0
        )
        wide = jnp.concatenate([jnp.where(low, maps, 0.0), jnp.where(low, 0.0, maps)], axis=0)
        scores = lax.dot_general(
            wide.astype(bf16),
            key_cache[b],
            (((1,), (1,)), ((), ())),
            preferred_element_type=f32,
        )
        past.append(jnp.where(place < lengths[b], scores * scale, -jnp.inf))
        selfs.append(jnp.sum(wide * keys[b : b + 1], axis=-1, keepdims=True) * scale)
    past = jnp.concatenate(past, axis=0)
    selfs = jnp.concatenate(selfs, axis=0)
    top = jnp.maximum(jnp.max(past, axis=-1, keepdims=True), selfs)
    past_exp = jnp.exp(past - top)
    self_exp = jnp.exp(selfs - top)
    share = 1.0 / (jnp.sum(past_exp, axis=-1, keepdims=True) + self_exp)
    past_prob = past_exp * share
    self_prob = self_exp * share
    copies[0].wait()
    values = jnp.dot(tokens[...], weight_here[...], preferred_element_type=f32)
    values = values.astype(bf16).astype(f32)
    copies[1].wait()
    copies[2].wait()
    outs = []
    for b in range(own):
        first, second, last = 2 * heads * b, 2 * heads * b + heads, 2 * heads * (b + 1)
        past_weight = (past_prob[first:second] - mixing * past_prob[second:last]).astype(bf16)
        self_weight = (self_prob[first:second] - mixing * self_prob[second:last]).astype(bf16)
        head_out = jnp.dot(past_weight, cache_here[b], preferred_element_type=f32)
        outs.append(head_out + self_weight.astype(f32) * values[b : b + 1])
    head_out = jnp.concatenate(outs, axis=0)
    spread = jnp.mean(head_out * head_out, axis=-1, keepdims=True)
    normed = head_out * lax.rsqrt(spread + EPS) * gain_here[...]
    rows = [
        jnp.concatenate([normed[b * heads + h : b * heads + h + 1] for h in range(heads)], axis=1)
        for b in range(own)
    ]
    attended[...] = jnp.concatenate(rows, axis=0).astype(bf16)


def expert_kernel(
    packed, gain, gate_weight, up_weight, down_weight, settled, terms, down_here, arrived
):
    copy = pltpu.make_async_copy(down_weight, down_here, arrived)
    copy.start()
    f32 = jnp.float32
    bf16 = jnp.bfloat16
    experts, tp_count, group, lanes = packed.shape
    part = lanes - LANES
    pieces = []
    for index in range(tp_count):
        piece = packed[:, index].astype(f32).reshape(experts * group, lanes)
        pieces.append(piece[:, :part] + (piece[:, part : part + 1] + piece[:, part + 1 : part + 2]))
    rows = norm_rows(jnp.concatenate(pieces, axis=1), gain[...]).astype(bf16)
    settled[...] = rows
    gate_h = jnp.dot(rows, gate_weight[...], preferred_element_type=f32)
    up_h = jnp.dot(rows, up_weight[...], preferred_element_type=f32)
    clipped = jnp.minimum(gate_h, LIMIT)
    linear = jnp.clip(up_h, -LIMIT, LIMIT)
    act = (clipped * jax.nn.sigmoid(SLOPE * clipped) * (linear + 1.0)).astype(bf16)
    copy.wait()
    terms[...] = jnp.dot(act, down_here[...], preferred_element_type=f32).astype(bf16)


def final_kernel(rank, settled, mine, other, gain, result, whole):
    f32 = jnp.float32
    part = result.shape[1]
    final = ALPHA * settled[...].astype(f32) + (mine[...] + other[...].astype(f32))
    mean = jnp.mean(final, axis=-1, keepdims=True)
    spread = jnp.mean((final - mean) * (final - mean), axis=-1, keepdims=True)
    whole[...] = (final - mean) * lax.rsqrt(spread + EPS) * gain[...]
    start = pl.multiple_of(rank[0] * part, LANES)
    result[...] = whole[:, pl.ds(start, part)].astype(jnp.bfloat16)


def body(
    tokens,
    lengths,
    key_cache,
    value_cache,
    query_weight,
    key_weight,
    value_weight,
    lambdas,
    head_gain,
    output_weight,
    norm1_gain,
    routes,
    route_logits,
    gate_weight,
    up_weight,
    down_weight,
    norm2_gain,
):
    bf16 = jnp.bfloat16
    f32 = jnp.float32
    tp_count = lax.axis_size("tp")
    tp_rank = lax.axis_index("tp")
    experts = lax.axis_size("ep")
    ep_rank = lax.axis_index("ep")
    own, width = tokens.shape
    group = own * tp_count
    part = width // tp_count
    heads = lambdas.shape[0]
    head_dim = key_weight.shape[1] // 2
    columns = query_weight.shape[1]
    cosine, sine = turns(lengths, head_dim // 2)
    own_turn = [lax.dynamic_slice_in_dim(t, tp_rank * own, own) for t in (cosine, sine)]
    if tp_count == 2:
        others = swap(tokens)
        peer_turn = [lax.dynamic_slice_in_dim(t, (1 - tp_rank) * own, own) for t in (cosine, sine)]
        sent = jnp.dot(others, query_weight, preferred_element_type=f32)
        sent = rotate(sent.reshape(own, -1, 2, head_dim), *peer_turn).astype(bf16)
        sent = sent.reshape(own, columns)
        late, sent = lax.optimization_barrier((tokens, sent))
        came = swap(sent)
        kept = jnp.dot(late, query_weight, preferred_element_type=f32)
        kept = rotate(kept.reshape(own, -1, 2, head_dim), *own_turn).astype(bf16)
        query = joined(kept.reshape(own, columns), came, tp_rank, 1)
        group_rows = joined(late, others, tp_rank, 0)
    else:
        late = tokens
        group_rows = lax.all_gather(tokens, "tp", axis=0, tiled=True)
        query = jnp.dot(group_rows, query_weight, preferred_element_type=f32)
        query = rotate(query.reshape(group, -1, 2, head_dim), cosine, sine).astype(bf16)
        query = lax.all_to_all(
            query.reshape(group, columns), "tp", split_axis=0, concat_axis=1, tiled=True
        )
    own_lengths = lax.dynamic_slice_in_dim(lengths, tp_rank * own, own)
    new_key = jnp.dot(late, key_weight, preferred_element_type=f32)
    new_key = new_key.reshape(own, 2, head_dim)
    new_key = rotate(new_key, *own_turn).astype(bf16).reshape(own, 2 * head_dim)
    attended = pl.pallas_call(
        attend_kernel,
        out_shape=jax.ShapeDtypeStruct((own, heads * value_cache.shape[2]), bf16),
        in_specs=[smem()] + [vmem()] * 5 + [away()] * 3,
        out_specs=vmem(),
        scratch_shapes=[
            pltpu.VMEM(value_weight.shape, bf16),
            pltpu.VMEM(value_cache.shape, bf16),
            pltpu.VMEM((1, value_cache.shape[2]), f32),
            pltpu.SemaphoreType.DMA((3,)),
        ],
        compiler_params=room(key_cache, value_cache, extra=2 << 20),
        name="attend",
    )(
        own_lengths,
        query,
        new_key,
        late,
        key_cache,
        lambdas.reshape(heads, 1),
        value_weight,
        value_cache,
        head_gain.reshape(1, -1),
    )
    zero = attended[0, 0].astype(f32) * 0.0
    gains = jnp.stack([norm1_gain, norm2_gain]) + zero
    gains = lax.optimization_barrier(gains)
    gathered = gather_tp(attended)
    mix = jnp.dot(gathered, output_weight, preferred_element_type=f32)
    column_start = tp_rank * part
    own_columns = lax.dynamic_slice_in_dim(group_rows, column_start, part, 1).astype(f32)
    summed = ALPHA * own_columns + mix
    part_mean = jnp.mean(summed, axis=1, keepdims=True)
    mean_high = part_mean.astype(bf16)
    mean_low = (part_mean - mean_high.astype(f32)).astype(bf16)
    lane = jnp.arange(LANES, dtype=jnp.int32)[None, :]
    extra = jnp.where(lane == 0, mean_high, jnp.where(lane == 1, mean_low, jnp.zeros((), bf16)))
    packed = jnp.concatenate([(summed - part_mean).astype(bf16), extra], axis=1)
    packed = jnp.broadcast_to(packed[None], (experts * tp_count,) + packed.shape)
    packed = lax.all_to_all(packed, ("ep", "tp"), split_axis=0, concat_axis=0, tiled=True)
    settled, terms = pl.pallas_call(
        expert_kernel,
        out_shape=(jax.ShapeDtypeStruct((experts * group, width), bf16),) * 2,
        in_specs=[vmem()] * 4 + [away()],
        out_specs=(vmem(), vmem()),
        scratch_shapes=[pltpu.VMEM(down_weight.shape[1:], bf16), pltpu.SemaphoreType.DMA],
        compiler_params=room(
            packed, gate_weight, up_weight, down_weight, extra=24 * experts * group * width
        ),
        name="expert",
    )(
        packed.reshape(experts, tp_count, group, part + LANES),
        gains[0:1],
        gate_weight[0],
        up_weight[0],
        down_weight[0],
    )
    terms = terms.reshape(experts, group, width)
    back = lax.all_to_all(terms, "ep", split_axis=0, concat_axis=0, tiled=True)
    route_weight = jax.nn.softmax(route_logits, axis=-1)
    names = jnp.arange(experts, dtype=jnp.int32)[:, None, None]
    dense = jnp.sum(jnp.where(routes[None] == names, route_weight[None], 0.0), axis=-1)
    mine = jnp.sum(back.astype(f32) * dense[:, :, None], axis=0)
    if tp_count == 2:
        other = swap(mine.astype(bf16))
    else:
        other = lax.psum(mine, "tp") - mine
    own_settled = lax.dynamic_slice_in_dim(settled, ep_rank * group, group)
    return pl.pallas_call(
        final_kernel,
        out_shape=jax.ShapeDtypeStruct((group, part), bf16),
        in_specs=[smem()] + [vmem()] * 4,
        out_specs=vmem(),
        scratch_shapes=[pltpu.VMEM((group, width), f32)],
        compiler_params=room(mine, mine, mine, extra=1 << 20),
        name="final",
    )(tp_rank.reshape(1), own_settled, mine, other, gains[1:2])


def solution(mesh):
    in_specs = (
        P(("ep", "tp"), None),
        P("ep"),
        P(("ep", "tp"), None, None),
        P(("ep", "tp"), None, None),
        P(None, "tp"),
        P(),
        P(),
        P(),
        P(),
        P(None, "tp"),
        P(),
        P("ep", None),
        P("ep", None),
        P("ep", None, "tp"),
        P("ep", None, "tp"),
        P("ep", "tp", None),
        P(),
    )
    out_specs = P("ep", "tp")

    return jax.shard_map(body, mesh=mesh, in_specs=in_specs, out_specs=out_specs, check_vma=False)
```
